32 devices in a mesh: kv: 16 (over z, y, x), tp: 2 (over core).
Axes of the slice: x: 2, y: 2, z: 4, core: 2. Of those that a mesh axis runs over, the one named last changes fastest.
Arguments:
- stream: bfloat16 [32, 4096], P(None, 'kv'), may hold values from -32 to 32
- gain_in: bfloat16 [4096], P('kv'), may hold values from 0.099609375 to 1.8984375
- w_query: bfloat16 [4096, 2048], P('kv', 'tp'), may hold values from -0.09375 to 0.09375
- w_key: bfloat16 [4096, 2048], P('kv', 'tp'), may hold values from -0.09375 to 0.09375
- w_value: bfloat16 [4096, 2048], P('kv', 'tp'), may hold values from -0.09375 to 0.09375
- w_forget: bfloat16 [4096, 16], replicated, may hold values from -0.09375 to 0.09375
- keys_cache: bfloat16 [32, 16, 2048, 128], P(None, 'tp', 'kv'), may hold values from -136 to 136
- values_cache: bfloat16 [32, 16, 2048, 128], P(None, 'tp', 'kv'), may hold values from -6 to 6
- decay_cache: float32 [32, 16, 2048], P(None, 'tp', 'kv'), may hold values from -323 to 0
- lengths: int32 [32], replicated, may hold values from 1 to 2048, 26246 in all
- gain_att: bfloat16 [2048], P('tp'), may hold values from 0.099609375 to 1.8984375
- w_out: bfloat16 [2048, 4096], P('tp', 'kv'), may hold values from -0.125 to 0.125
- gain_mlp: bfloat16 [4096], P('kv'), may hold values from 0.099609375 to 1.8984375
- w_up: bfloat16 [4096, 16384], P('kv', 'tp'), may hold values from -0.09375 to 0.09375
- w_down: bfloat16 [16384, 4096], P('tp', 'kv'), may hold values from -0.046875 to 0.046875
Outputs:
- updated: bfloat16 [32, 4096], P(None, 'kv')
The draws below stay inside these ranges and needn't reach their ends.
Inputs may be any that keep to these rules, and one draw needn't show every extreme that they name: `lengths`: one sequence has all 2048 positions live.
All inputs are finite; a program needn't handle non-finite values.
Results may differ from the reference program's by a relative error of at most 0.012.
The reference program's roundings to bfloat16 on the way count: a program that leaves them out, or rounds other values in their place, can miss the bound.
Values may be sent and summed in bfloat16 or wider, within the bound.
A program may use at most 64 MiB of HBM per device.

```python
import math
import jax
import jax.numpy as jnp
import numpy as np
from jax import lax

D = 4096
HEAD_COUNT = 16
HEAD_WIDTH = 128
FF = 16384
SEQUENCE_COUNT = 32
POS_DEV = 128
CACHE_LENGTH = 2048
HW = 2048


def draw_stream(key, part):
    key_one, key_two = jax.random.split(jax.random.fold_in(key, 11), 2)
    column = jnp.arange(D, dtype=jnp.float32) / D
    raw_values = jnp.clip(jax.random.normal(key_one, (SEQUENCE_COUNT, D), jnp.float32), -5.0, 5.0)
    column_scale = jnp.exp(math.log(10.0) * (column - 0.5))
    row_scale = jnp.exp(jax.random.uniform(key_two, (SEQUENCE_COUNT, 1), jnp.float32, math.log(0.5), math.log(2.0)))
    return (raw_values * column_scale[None, :] * row_scale).astype(jnp.bfloat16)


def draw_keys_cache(key, part):
    key_one = jax.random.fold_in(jax.random.fold_in(key, 5), 0)
    full_shape = (SEQUENCE_COUNT, HEAD_COUNT, CACHE_LENGTH, HEAD_WIDTH)
    raw_values = jnp.clip(jax.random.normal(key_one, full_shape, jnp.float32), -5.0, 5.0)
    return raw_values.astype(jnp.bfloat16)


def draw_decay_cache(key, part):
    every_key = jax.random.split(jax.random.fold_in(key, 23), 7)
    head_order = jax.random.permutation(every_key[0], HEAD_COUNT)
    keep_count = HEAD_COUNT // 2
    slow_heads = (head_order < keep_count).reshape(1, HEAD_COUNT, 1)
    slow_rate = jax.random.uniform(every_key[1], (SEQUENCE_COUNT, HEAD_COUNT, 1), jnp.float32, 0.2, 0.8) / CACHE_LENGTH
    fast_rate = 1.0 / (POS_DEV * jax.random.uniform(every_key[2], (SEQUENCE_COUNT, HEAD_COUNT, 1), jnp.float32, 0.25, 0.8))
    learning_rate = jnp.where(slow_heads, slow_rate, fast_rate)
    jaggedness = jnp.exp(jax.random.uniform(every_key[3], (SEQUENCE_COUNT, HEAD_COUNT, CACHE_LENGTH), jnp.float32, math.log(0.5), math.log(2.0)))
    block_count = CACHE_LENGTH // POS_DEV
    block_multiplier = jnp.exp(jax.random.uniform(every_key[4], (1, HEAD_COUNT, block_count, 1), jnp.float32, math.log(0.4), math.log(2.5)))
    block_multiplier = jnp.broadcast_to(block_multiplier, (1, HEAD_COUNT, block_count, POS_DEV)).reshape(1, HEAD_COUNT, CACHE_LENGTH)
    spike_position = jax.random.randint(every_key[5], (SEQUENCE_COUNT, HEAD_COUNT, 3, 1), 0, CACHE_LENGTH)
    spike_penalty = jnp.log(jax.random.uniform(every_key[6], (SEQUENCE_COUNT, HEAD_COUNT, 3, 1), jnp.float32, 0.5, 0.8))
    cache_positions = jnp.arange(CACHE_LENGTH, dtype=jnp.int32)
    spike_events = jnp.sum(jnp.where(cache_positions[None, None, None, :] == spike_position, spike_penalty, 0.0), axis=2)
    gate_logarithms = spike_events - learning_rate * jaggedness * block_multiplier
    suffix_sum = jnp.flip(jnp.cumsum(jnp.flip(gate_logarithms, 2), axis=2), 2)
    return suffix_sum - gate_logarithms


def shard_levels(own_key, extent, cuts, least, high):
    factor_of = 1.0
    for dim, shards_of in cuts:
        steps = jax.random.uniform(jax.random.fold_in(jax.random.fold_in(own_key, 6), dim), (shards_of,), jnp.float32, least / len(cuts), high / len(cuts))
        factor_of = factor_of * jnp.repeat(jnp.exp(steps), extent[dim] // shards_of).reshape((-1,) + (1,) * (len(extent) - 1 - dim))
    return factor_of


def profile(amount, total, bound, skew):
    portions = [(1 << 20) // math.isqrt(grade ** skew) + 1 for grade in range(2, amount + 1)]
    rest, given = total - bound - (amount - 1), [1] * (amount - 1)
    while rest > 0:
        movable = [i for i in range(amount - 1) if given[i] < bound]
        whole, budget = sum([portions[i] for i in movable]), rest
        for i in movable:
            extra = min(bound - given[i], max(1, budget * portions[i] // whole), rest)
            given[i] = given[i] + extra
            rest = rest - extra
    return np.array([bound] + given)


def ragged(stream_key, count, total, reach, slope):
    if count == 2:
        one = jax.random.randint(stream_key, (), max(1, total - reach), min(reach, total - 1) + 1)
        return jnp.stack([one, total - one])
    tallies = jnp.asarray(profile(count, total, reach, slope), jnp.int32)
    couples = (count - 1) // 2
    source_of, receiver = tallies[1:1 + 2 * couples:2], tallies[2:2 + 2 * couples:2]
    slack = jnp.minimum(source_of - 1, reach - receiver)
    moved = jax.random.randint(jax.random.fold_in(stream_key, 1), (couples,), 0, 1 << 20) % (slack + 1)
    tallies = tallies.at[1:1 + 2 * couples:2].set(source_of - moved).at[2:2 + 2 * couples:2].set(receiver + moved)
    return tallies[jax.random.permutation(jax.random.fold_in(stream_key, 2), count)]


def noise(key, dims, spread, bound, shards=(), kind=jnp.bfloat16):
    entries = spread * jax.random.normal(key, dims, jnp.float32)
    if shards:
        entries = entries * shard_levels(key, dims, shards, -0.22, 0.18)
    return jnp.clip(entries, -bound, bound).astype(kind)


def setup_inputs(seed: int = 0) -> dict:
    splits = jax.random.split(jax.random.key(seed), 16)
    stream = draw_stream(jax.random.fold_in(splits[15], 71), 0)
    gain_in = jnp.clip(1.0 + 0.18 * jax.random.normal(splits[1], (D,), jnp.float32), 0.099609375, 1.8984375).astype(jnp.bfloat16)
    w_query = noise(splits[2], (D, HW), D ** -0.5, 0.09375, ((0, 16), (1, 2)))
    w_key = noise(splits[3], (D, HW), D ** -0.5, 0.09375, ((0, 16), (1, 2)))
    w_value = noise(splits[4], (D, HW), D ** -0.5, 0.09375, ((0, 16), (1, 2)))
    w_forget = noise(splits[5], (D, HEAD_COUNT), D ** -0.5, 0.09375)
    keys_cache = draw_keys_cache(jax.random.fold_in(splits[15], 71), 0)
    values_cache = noise(splits[7], (SEQUENCE_COUNT, HEAD_COUNT, CACHE_LENGTH, HEAD_WIDTH), 1.0, 6.0, ((1, 2), (2, 16)))
    decay_cache = draw_decay_cache(jax.random.fold_in(splits[15], 71), 0)
    lengths = ragged(splits[9], SEQUENCE_COUNT, SEQUENCE_COUNT * CACHE_LENGTH * 2 // 5 + SEQUENCE_COUNT, CACHE_LENGTH, 2).astype(jnp.int32)
    gain_att = jnp.clip(1.0 + 0.18 * jax.random.normal(splits[10], (HW,), jnp.float32), 0.099609375, 1.8984375).astype(jnp.bfloat16)
    w_out = noise(splits[11], (HW, D), HW ** -0.5, 0.125, ((0, 2), (1, 16)))
    gain_mlp = jnp.clip(1.0 + 0.18 * jax.random.normal(splits[12], (D,), jnp.float32), 0.099609375, 1.8984375).astype(jnp.bfloat16)
    w_up = noise(splits[13], (D, FF), D ** -0.5, 0.09375, ((0, 16), (1, 2)))
    w_down = noise(splits[14], (FF, D), FF ** -0.5, 0.046875, ((0, 2), (1, 16)))
    return {"stream": stream, "gain_in": gain_in, "w_query": w_query, "w_key": w_key, "w_value": w_value, "w_forget": w_forget, "keys_cache": keys_cache, "values_cache": values_cache, "decay_cache": decay_cache, "lengths": lengths, "gain_att": gain_att, "w_out": w_out, "gain_mlp": gain_mlp, "w_up": w_up, "w_down": w_down}


norm_eps = 1e-06
masked_score = -1e+30

def head_blocks(head_index, queries, forget, keys_cache, values_cache, decay_cache, lengths):
    block_count = CACHE_LENGTH // POS_DEV
    head_queries = lax.dynamic_index_in_dim(queries, head_index, 1, False).astype(jnp.float32)
    head_keys = lax.dynamic_index_in_dim(keys_cache, head_index, 1, False).astype(jnp.float32)
    value_head = lax.dynamic_index_in_dim(values_cache, head_index, 1, False).astype(jnp.float32)
    decay_head = lax.dynamic_index_in_dim(decay_cache, head_index, 1, False)
    forget_head = lax.dynamic_index_in_dim(forget, head_index, 1, False)
    attention_logits = jnp.einsum('tk,txk->tx', head_queries, head_keys) * (1.0 / math.sqrt(HEAD_WIDTH))
    attention_logits = attention_logits + forget_head[:, None] + decay_head
    attention_logits = attention_logits.reshape(SEQUENCE_COUNT, block_count, POS_DEV)
    cache_positions = jnp.arange(CACHE_LENGTH, dtype=jnp.int32).reshape(block_count, POS_DEV)
    live_mask = cache_positions[None] < lengths.astype(jnp.int32)[:, None, None]
    attention_logits = jnp.where(live_mask, attention_logits, masked_score)
    block_peak = lax.optimization_barrier(jnp.max(attention_logits, axis=2))
    weights = jnp.where(live_mask, jnp.exp(attention_logits - block_peak[..., None]), 0.0)
    block_total = lax.optimization_barrier(jnp.sum(weights, axis=2))
    rounded = lax.optimization_barrier(weights.astype(jnp.bfloat16)).astype(jnp.float32)
    block_out = jnp.einsum('sbp,sbpd->sbd', rounded, value_head.reshape(SEQUENCE_COUNT, block_count, POS_DEV, HEAD_WIDTH))
    return (block_peak, block_total, block_out)

def reference(stream, gain_in, w_query, w_key, w_value, w_forget, keys_cache, values_cache, decay_cache, lengths, gain_att, w_out, gain_mlp, w_up, w_down):
    score_scale = 1.0 / math.sqrt(HEAD_WIDTH)
    stream_float = stream.astype(jnp.float32)
    scaled = (stream_float * gain_in.astype(jnp.float32)).astype(jnp.bfloat16)
    scale_in = lax.rsqrt(lax.optimization_barrier(jnp.mean(stream_float * stream_float, axis=1)) + norm_eps)[:, None]
    queries = (jnp.dot(scaled, w_query, preferred_element_type=jnp.float32) * scale_in).astype(jnp.bfloat16).reshape(SEQUENCE_COUNT, HEAD_COUNT, HEAD_WIDTH)
    key_new = (jnp.dot(scaled, w_key, preferred_element_type=jnp.float32) * scale_in).astype(jnp.bfloat16).reshape(SEQUENCE_COUNT, HEAD_COUNT, HEAD_WIDTH)
    value_new = (jnp.dot(scaled, w_value, preferred_element_type=jnp.float32) * scale_in).astype(jnp.bfloat16).reshape(SEQUENCE_COUNT, HEAD_COUNT, HEAD_WIDTH)
    forget = jax.nn.log_sigmoid(jnp.dot(scaled, w_forget, preferred_element_type=jnp.float32) * scale_in)
    block_peaks, totals, block_outs = lax.map(lambda head_index: head_blocks(head_index, queries, forget, keys_cache, values_cache, decay_cache, lengths), jnp.arange(HEAD_COUNT, dtype=jnp.int32))
    block_peaks = jnp.transpose(block_peaks, (1, 0, 2))
    totals = jnp.transpose(totals, (1, 0, 2))
    block_outs = jnp.transpose(block_outs, (1, 0, 2, 3))
    own_score = lax.optimization_barrier(jnp.sum(queries.astype(jnp.float32) * key_new.astype(jnp.float32), axis=2)) * score_scale
    top_score = jnp.maximum(lax.optimization_barrier(jnp.max(block_peaks, axis=2)), own_score)
    block_weight = jnp.exp(block_peaks - top_score[..., None])
    own_weight = jnp.exp(own_score - top_score)
    numerator = lax.optimization_barrier(jnp.sum(block_weight[..., None] * block_outs, axis=2)) + own_weight[..., None] * value_new.astype(jnp.float32)
    denominator = lax.optimization_barrier(jnp.sum(block_weight * totals, axis=2)) + own_weight
    attended = (numerator / denominator[..., None]).reshape(SEQUENCE_COUNT, HW)
    scale_att = lax.rsqrt(lax.optimization_barrier(jnp.mean(attended * attended, axis=1)) + norm_eps)[:, None]
    attended_in = (attended * gain_att.astype(jnp.float32)).astype(jnp.bfloat16)
    residual = (stream_float + scale_att * jnp.dot(attended_in, w_out, preferred_element_type=jnp.float32)).astype(jnp.bfloat16)
    residual_float = residual.astype(jnp.float32)
    mixer_in = (residual_float * gain_mlp.astype(jnp.float32)).astype(jnp.bfloat16)
    scale_mixer = lax.rsqrt(lax.optimization_barrier(jnp.mean(residual_float * residual_float, axis=1)) + norm_eps)[:, None]
    hidden = jnp.square(jax.nn.relu(jnp.dot(mixer_in, w_up, preferred_element_type=jnp.float32) * scale_mixer)).astype(jnp.bfloat16)
    return (residual_float + jnp.dot(hidden, w_down, preferred_element_type=jnp.float32)).astype(jnp.bfloat16)
```

```python
import functools
import math

import jax
import jax.numpy as jnp
from jax import lax
from jax.experimental import pallas as pl
from jax.experimental.pallas import tpu as pltpu
from jax.sharding import PartitionSpec as P

f32 = jnp.float32
bf16 = jnp.bfloat16
LANES = 128

norm_eps = 1e-06
masked_score = -1e30


def merged_2(value, axis, join):
    pieces = jax.tree.map(lambda part: lax.all_gather(part, axis), value)
    head = jax.tree.map(lambda part: part[0], pieces)
    tail = jax.tree.map(lambda part: part[1:], pieces)
    so_far, _ = lax.scan(lambda so_far, share: (join(so_far, share), None), head, tail)
    return so_far


def fold_parts(left_part, right_part):
    peak_all = jnp.maximum(left_part[0], right_part[0])
    weight_one = jnp.exp(left_part[0] - peak_all)
    weight_two = jnp.exp(right_part[0] - peak_all)
    total_sum = left_part[1] * weight_one + right_part[1] * weight_two
    merged = left_part[2] * weight_one[..., None] + right_part[2] * weight_two[..., None]
    return (peak_all, total_sum, merged)


def per_device(
    stream,
    gain_in,
    w_query,
    w_key,
    w_value,
    w_forget,
    keys_cache,
    values_cache,
    decay_cache,
    lengths,
    gain_att,
    w_out,
    gain_mlp,
    w_up,
    w_down,
):
    kv_index = lax.axis_index("kv")
    tp_index = lax.axis_index("tp")
    kv_count = lax.axis_size("kv")
    seqs_here, cols_here = stream.shape
    heads_here = keys_cache.shape[1]
    pos_here = keys_cache.shape[2]
    head_dim = keys_cache.shape[3]
    width_all = cols_here * kv_count
    score_scale = 1.0 / math.sqrt(head_dim)
    stream_float = stream.astype(jnp.float32)
    scaled = (stream_float * gain_in.astype(jnp.float32)).astype(jnp.bfloat16)
    square_sum = jnp.sum(stream_float * stream_float, axis=1)
    forget_rows = lax.dynamic_slice(
        w_forget, (kv_index * cols_here, tp_index * heads_here), (cols_here, heads_here)
    )
    part_query = jnp.dot(scaled, w_query, preferred_element_type=jnp.float32)
    part_key = jnp.dot(scaled, w_key, preferred_element_type=jnp.float32)
    part_value = jnp.dot(scaled, w_value, preferred_element_type=jnp.float32)
    part_forget = jnp.dot(scaled, forget_rows, preferred_element_type=jnp.float32)
    part_query, part_key, part_value, part_forget, square_total = lax.psum(
        (part_query, part_key, part_value, part_forget, square_sum), "kv"
    )
    scale_in = lax.rsqrt(square_total / width_all + norm_eps)[:, None]
    queries = (part_query * scale_in).astype(jnp.bfloat16).reshape(seqs_here, heads_here, head_dim)
    key_new = (part_key * scale_in).astype(jnp.bfloat16).reshape(seqs_here, heads_here, head_dim)
    value_new = (
        (part_value * scale_in).astype(jnp.bfloat16).reshape(seqs_here, heads_here, head_dim)
    )
    forget = jax.nn.log_sigmoid(part_forget * scale_in)
    attention_logits = (
        jnp.einsum("shd,shpd->shp", queries, keys_cache, preferred_element_type=jnp.float32)
        * score_scale
    )
    attention_logits = attention_logits + forget[:, :, None] + decay_cache
    cache_positions = kv_index * pos_here + lax.iota(jnp.int32, pos_here)
    live_mask = (cache_positions[None, :] < lengths[:, None])[:, None, :]
    attention_logits = jnp.where(live_mask, attention_logits, masked_score)
    block_peak = jnp.max(attention_logits, axis=2)
    weights = jnp.where(live_mask, jnp.exp(attention_logits - block_peak[..., None]), 0.0)
    block_total = jnp.sum(weights, axis=2)
    block_out = jnp.einsum(
        "shp,shpd->shd",
        weights.astype(jnp.bfloat16),
        values_cache,
        preferred_element_type=jnp.float32,
    )
    peak_all, total_all, out_all = merged_2((block_peak, block_total, block_out), "kv", fold_parts)
    own_score = (
        jnp.sum(queries.astype(jnp.float32) * key_new.astype(jnp.float32), axis=2) * score_scale
    )
    top_score = jnp.maximum(peak_all, own_score)
    past_weight = jnp.exp(peak_all - top_score)
    own_weight = jnp.exp(own_score - top_score)
    numerator = (
        out_all * past_weight[..., None] + value_new.astype(jnp.float32) * own_weight[..., None]
    )
    denominator = total_all * past_weight + own_weight
    attended = (numerator / denominator[..., None]).reshape(seqs_here, heads_here * head_dim)
    attended_in = (attended * gain_att.astype(jnp.float32)).astype(jnp.bfloat16)
    part_out = jnp.dot(attended_in, w_out, preferred_element_type=jnp.float32)
    att_squares = jnp.sum(attended * attended, axis=1)
    part_out, att_total = lax.psum((part_out, att_squares), "tp")
    scale_att = lax.rsqrt(att_total / (attended.shape[1] * lax.axis_size("tp")) + norm_eps)[:, None]
    residual = (stream_float + scale_att * part_out).astype(jnp.bfloat16)
    residual_float = residual.astype(jnp.float32)
    mixer_in = (residual_float * gain_mlp.astype(jnp.float32)).astype(jnp.bfloat16)
    mixer_squares = jnp.sum(residual_float * residual_float, axis=1)
    part_up = jnp.dot(mixer_in, w_up, preferred_element_type=jnp.float32)
    pre_act, mixer_total = lax.psum((part_up, mixer_squares), "kv")
    scale_mixer = lax.rsqrt(mixer_total / width_all + norm_eps)[:, None]
    hidden = jnp.square(jax.nn.relu(pre_act * scale_mixer)).astype(jnp.bfloat16)
    part_down = jnp.dot(hidden, w_down, preferred_element_type=jnp.float32)
    mixer_out = lax.psum(part_down, "tp")
    return (residual_float + mixer_out).astype(jnp.bfloat16)


def thirds(value, group, wide):
    high = value.astype(bf16).astype(f32)
    rest = value - high
    mid = rest.astype(bf16).astype(f32)
    low = rest - mid
    third = group % 3 if wide else group
    picked = jnp.where(third == 0, high, jnp.where(third == 1, mid, low))
    return picked


def lanes_of(shape):
    return lax.broadcasted_iota(jnp.int32, shape, len(shape) - 1)


def layer_kernel(
    kv_n, heads_all, pos_here,
    lengths, stream, gain_in, gain_att, gain_mlp, decay,
    w_forget, w_query, w_key, w_value, keys, values, w_out, w_up, w_down,
    out,
    wf_v, wq_v, wk_v, wv_v, keys_v, values_v, wo_v, wu_v, wd_v,
    send1, recv1, q_all, q_float, o_float, s_float, send3, recv3, att_all,
    send5, recv5, send6, recv6, hid_all, send8, recv8,
    load_sem, cache_sem, ssem, rsem, pair_ssem, pair_rsem,
):
    me = lax.axis_index("kv")
    tp = lax.axis_index("tp")
    seqs, cols = stream.shape
    heads = decay.shape[1]
    dim = keys.shape[-1]
    rows = send1.shape[1] // 4
    groups = seqs // rows
    hidden_here = hid_all.shape[2]
    others = kv_n - 1
    chunks = cache_sem.shape[1]
    per_chunk = seqs // chunks
    score_scale = 1.0 / math.sqrt(dim)

    def load(src, dst, index):
        return pltpu.make_async_copy(src, dst, load_sem.at[index])

    start_row = pl.multiple_of(me * cols, cols)
    first_loads = [
        load(w_forget.at[pl.ds(start_row, cols), :], wf_v, 0),
        load(w_query, wq_v, 1),
        load(w_key, wk_v, 2),
        load(w_value, wv_v, 3),
    ]
    for copy in first_loads:
        copy.start()

    def cache_copy(which, chunk):
        src, dst = ((keys, keys_v), (values, values_v))[which]
        part = pl.ds(chunk * per_chunk, per_chunk)
        return pltpu.make_async_copy(src.at[part], dst.at[part], cache_sem.at[which, chunk])

    late_loads = [load(w_out, wo_v, 4), load(w_up, wu_v, 5), load(w_down, wd_v, 6)]

    barrier = pltpu.get_barrier_semaphore()

    def greet(k, carry):
        pl.semaphore_signal(
            barrier, inc=1, device_id=(lax.rem(me + k, kv_n), tp),
            device_id_type=pl.DeviceIdType.MESH,
        )
        return carry

    lax.fori_loop(1, kv_n, greet, 0)
    pl.semaphore_signal(
        barrier, inc=1, device_id=(me, 1 - tp), device_id_type=pl.DeviceIdType.MESH
    )

    def after(k):
        return lax.rem(me + k, kv_n)

    def before(k):
        return lax.rem(me + kv_n - k, kv_n)

    def remote(phase, k, src, dst):
        return pltpu.make_async_remote_copy(
            src_ref=src, dst_ref=dst,
            send_sem=ssem.at[phase, k - 1], recv_sem=rsem.at[phase, k - 1],
            device_id=(after(k), tp), device_id_type=pl.DeviceIdType.MESH,
        )

    def scatter(phase, k, send, recv):
        return remote(phase, k, send.at[after(k)], recv.at[k - 1])

    def spread(phase, k, held):
        return remote(phase, k, held.at[me], held.at[me])

    def landed(phase, k, held):
        return remote(phase, k, held.at[before(k)], held.at[before(k)])

    def each(body):
        lax.fori_loop(1, kv_n, lambda k, carry: (body(k), carry)[1], 0)

    def swap(index, src, dst):
        return pltpu.make_async_remote_copy(
            src_ref=src, dst_ref=dst, send_sem=pair_ssem.at[index],
            recv_sem=pair_rsem.at[index], device_id=(me, 1 - tp),
            device_id_type=pl.DeviceIdType.MESH,
        )

    x = stream[...].astype(f32)
    scaled = (x * gain_in[...].astype(f32)).astype(bf16)
    squares = jnp.sum(x * x, axis=1, keepdims=True)
    for copy in first_loads:
        copy.wait()
    for chunk in range(chunks):
        cache_copy(0, chunk).start()
        cache_copy(1, chunk).start()
    for copy in late_loads:
        copy.start()
    lane = lanes_of((seqs, LANES))
    expand = lax.broadcasted_iota(jnp.int32, (heads_all, LANES), 0) == (
        lanes_of((heads_all, LANES)) % 32
    )
    wide_forget = jnp.dot(
        wf_v[...], jnp.where(expand, 1.0, 0.0).astype(bf16), preferred_element_type=f32
    ).astype(bf16)
    part_forget = jnp.dot(scaled, wide_forget, preferred_element_type=f32)
    stats = jnp.where(lane % 32 < heads_all, part_forget, squares)
    stats = thirds(stats, lane // 32, False)
    stats = jnp.where(lane < 96, stats, 0.0).astype(bf16)
    for place, weight in enumerate((wq_v, wk_v, wv_v)):
        part = jnp.dot(scaled, weight[...], preferred_element_type=f32).astype(bf16)
        for g in range(groups):
            for h in range(heads):
                send1[g * heads + h, place * rows:(place + 1) * rows, :] = part[
                    g * rows:(g + 1) * rows, h * dim:(h + 1) * dim
                ]
    for g in range(groups):
        for h in range(heads):
            send1[g * heads + h, 3 * rows:4 * rows, :] = stats[g * rows:(g + 1) * rows]
    pl.semaphore_wait(barrier, kv_n)
    each(lambda k: scatter(0, k, send1, recv1).start())

    def add1(k, total):
        scatter(0, k, send1, recv1).wait_recv()
        return total + recv1[k - 1].astype(f32)

    total = lax.fori_loop(1, kv_n, add1, send1[me].astype(f32))
    lane_r = lanes_of((rows, LANES))
    stat = total[3 * rows:]
    my_head = tp * heads + lax.rem(me, heads)
    forget_sum = jnp.sum(
        jnp.where(lane_r % 32 == my_head, stat, 0.0), axis=1, keepdims=True
    )
    square_sum = jnp.sum(
        jnp.where(lane_r % 32 == heads_all, stat, 0.0), axis=1, keepdims=True
    )
    width_all = cols * kv_n
    scale_in = lax.rsqrt(square_sum / width_all + norm_eps)
    query = (total[:rows] * scale_in).astype(bf16)
    key_new = (total[rows:2 * rows] * scale_in).astype(bf16).astype(f32)
    value_new = (total[2 * rows:3 * rows] * scale_in).astype(bf16).astype(f32)
    gate = forget_sum * scale_in
    forget = jnp.minimum(gate, 0.0) - jnp.log1p(jnp.exp(-jnp.abs(gate)))
    q_all[me] = query
    each(lambda k: spread(1, k, q_all).start())
    own_score = (
        jnp.sum(query.astype(f32) * key_new, axis=1, keepdims=True) * score_scale
    )
    each(lambda k: landed(1, k, q_all).wait_recv())

    q_float[...] = q_all[...].reshape(kv_n * rows, dim).astype(f32)
    head_row = lax.broadcasted_iota(jnp.int32, (heads, pos_here), 0)
    position = me * pos_here + lanes_of((heads, pos_here))
    lane_h = lanes_of((heads, LANES))

    def one_sequence(s):
        first = (s // rows) * (heads * rows) + s % rows
        mine = pl.ds(first, heads, stride=rows)
        q_s = q_float[mine, :].astype(bf16)
        k_s = keys_v[s].reshape(heads * pos_here, dim)
        every = lax.dot_general(
            q_s, k_s, (((1,), (1,)), ((), ())), preferred_element_type=f32
        )
        score = every[:, :pos_here]
        for h in range(1, heads):
            score = jnp.where(
                head_row == h, every[:, h * pos_here:(h + 1) * pos_here], score
            )
        score = score * score_scale + decay[s]
        live = position < lengths[s]
        score = jnp.where(live, score, masked_score)
        peak = jnp.max(score, axis=1, keepdims=True)
        probs = jnp.where(live, jnp.exp(score - peak), 0.0)
        block_total = jnp.sum(probs, axis=1, keepdims=True)
        spread_probs = jnp.concatenate(
            [jnp.where(head_row == h, probs, 0.0) for h in range(heads)], axis=1
        ).astype(bf16)
        v_s = values_v[s].reshape(heads * pos_here, dim)
        o_float[mine, :] = jnp.dot(spread_probs, v_s, preferred_element_type=f32)
        s_float[mine, :] = jnp.where(lane_h < 48, peak, block_total)

    def one_chunk(chunk, carry):
        cache_copy(0, chunk).wait()
        cache_copy(1, chunk).wait()

        def inner(i, c):
            one_sequence(chunk * per_chunk + 2 * i)
            one_sequence(chunk * per_chunk + 2 * i + 1)
            return c

        return lax.fori_loop(0, per_chunk // 2, inner, carry)

    lax.fori_loop(0, chunks, one_chunk, 0)
    stats3 = s_float[...]
    stats3 = thirds(stats3, lanes_of(stats3.shape) // 16, True)
    send3[:, :rows, :] = o_float[...].astype(bf16).reshape(kv_n, rows, dim)
    send3[:, rows:, :] = stats3.astype(bf16).reshape(kv_n, rows, LANES)
    each(lambda k: scatter(2, k, send3, recv3).start())

    def opened(block):
        wide = block.astype(f32)
        stat = wide[rows:]
        is_third = lane_r % 16 == 0
        peak = jnp.sum(
            jnp.where(is_third & (lane_r < 48), stat, 0.0), axis=1, keepdims=True
        )
        total = jnp.sum(
            jnp.where(is_third & (lane_r >= 48) & (lane_r < 96), stat, 0.0),
            axis=1, keepdims=True,
        )
        return peak, total, wide[:rows]

    def fold3(k, so_far):
        scatter(2, k, send3, recv3).wait_recv()
        peak_a, total_a, out_a = so_far
        peak_b, total_b, out_b = opened(recv3[k - 1])
        peak = jnp.maximum(peak_a, peak_b)
        one, two = jnp.exp(peak_a - peak), jnp.exp(peak_b - peak)
        return peak, total_a * one + total_b * two, out_a * one + out_b * two

    peak_all, total_all, out_all = lax.fori_loop(1, kv_n, fold3, opened(send3[me]))
    peak_all = peak_all + forget
    top = jnp.maximum(peak_all, own_score)
    past_weight = jnp.exp(peak_all - top)
    own_weight = jnp.exp(own_score - top)
    att_all[me] = (out_all * past_weight + value_new * own_weight) / (
        total_all * past_weight + own_weight
    )
    each(lambda k: spread(3, k, att_all).start())
    each(lambda k: landed(3, k, att_all).wait_recv())
    attended = jnp.concatenate(
        [
            jnp.concatenate([att_all[g * heads + h] for g in range(groups)], axis=0)
            for h in range(heads)
        ],
        axis=1,
    )
    attended_in = (attended * gain_att[...].astype(f32)).astype(bf16)
    late_loads[0].wait()
    part_out = jnp.dot(attended_in, wo_v[...], preferred_element_type=f32)
    att_squares = jnp.sum(attended * attended, axis=1, keepdims=True)
    send5[:, :cols] = part_out
    send5[:, cols:] = jnp.broadcast_to(att_squares, (seqs, LANES))
    swap5 = swap(0, send5, recv5)
    swap5.start()
    late_loads[1].wait()
    swap5.wait_recv()
    scale_att = lax.rsqrt(
        (att_squares + recv5[:, cols:cols + 1]) / (attended.shape[1] * 2) + norm_eps
    )
    residual = (
        stream[...].astype(f32) + scale_att * (part_out + recv5[:, :cols])
    ).astype(bf16).astype(f32)
    mixer_in = (residual * gain_mlp[...].astype(f32)).astype(bf16)
    mixer_squares = jnp.sum(residual * residual, axis=1, keepdims=True)
    mixer_stats = thirds(jnp.broadcast_to(mixer_squares, (seqs, LANES)), lane, False)
    mixer_stats = jnp.where(lane < 3, mixer_stats, 0.0).astype(bf16)

    def up(owner):
        columns = pl.ds(pl.multiple_of(owner * hidden_here, LANES), hidden_here)
        send6[owner, :, :hidden_here] = jnp.dot(
            mixer_in, wu_v[:, columns], preferred_element_type=f32
        ).astype(bf16)
        send6[owner, :, hidden_here:] = mixer_stats

    def up_send(k):
        up(after(k))
        scatter(4, k, send6, recv6).start()

    each(up_send)
    up(me)

    def add6(k, total):
        scatter(4, k, send6, recv6).wait_recv()
        return total + recv6[k - 1].astype(f32)

    pre_act = lax.fori_loop(1, kv_n, add6, send6[me].astype(f32))
    mixer_total = jnp.sum(pre_act[:, hidden_here:], axis=1, keepdims=True)
    scale_mixer = lax.rsqrt(mixer_total / width_all + norm_eps)
    hidden = jnp.maximum(pre_act[:, :hidden_here] * scale_mixer, 0.0)
    hid_all[me] = (hidden * hidden).astype(bf16)
    each(lambda k: spread(5, k, hid_all).start())
    late_loads[2].wait()

    def down(owner):
        depth = pl.ds(pl.multiple_of(owner * hidden_here, LANES), hidden_here)
        return jnp.dot(hid_all[owner], wd_v[depth, :], preferred_element_type=f32)

    def add7(k, total):
        landed(5, k, hid_all).wait_recv()
        return total + down(before(k))

    part_down = lax.fori_loop(1, kv_n, add7, down(me))
    send8[...] = part_down
    swap8 = swap(1, send8, recv8)
    swap8.start()
    swap8.wait_recv()
    out[...] = (residual + (part_down + recv8[...])).astype(bf16)

    def drain(k):
        scatter(0, k, send1, recv1).wait_send()
        spread(1, k, q_all).wait_send()
        scatter(2, k, send3, recv3).wait_send()
        spread(3, k, att_all).wait_send()
        scatter(4, k, send6, recv6).wait_send()
        spread(5, k, hid_all).wait_send()

    each(drain)
    swap5.wait_send()
    swap8.wait_send()


def fits(kv_n, tp_n, seqs, cols, heads, heads_all, pos_here, dim, units):
    if tp_n != 2 or heads != 8 or (seqs * heads) % kv_n or units % kv_n:
        return False
    rows = seqs * heads // kv_n
    return (
        rows % 16 == 0 and seqs % rows == 0 and seqs % 16 == 0 and cols % LANES == 0
        and pos_here == LANES and dim == LANES and heads_all <= 16
        and (units // kv_n) % LANES == 0
    )


def layer(
    stream, gain_in, w_query, w_key, w_value, w_forget, keys_cache, values_cache,
    decay_cache, lengths, gain_att, w_out, gain_mlp, w_up, w_down,
):
    kv_n, tp_n = lax.axis_size("kv"), lax.axis_size("tp")
    seqs, cols = stream.shape
    heads, pos_here, dim = keys_cache.shape[1:]
    heads_all = w_forget.shape[1]
    units = w_up.shape[1]
    if not fits(kv_n, tp_n, seqs, cols, heads, heads_all, pos_here, dim, units):
        return per_device(
            stream, gain_in, w_query, w_key, w_value, w_forget, keys_cache, values_cache,
            decay_cache, lengths, gain_att, w_out, gain_mlp, w_up, w_down,
        )
    rows = seqs * heads // kv_n
    hidden_here = units // kv_n
    others = kv_n - 1
    chunks = 4 if seqs % 8 == 0 else 1
    vmem = pl.BlockSpec(memory_space=pltpu.VMEM)
    anywhere = pl.BlockSpec(memory_space=pl.ANY)
    return pl.pallas_call(
        functools.partial(layer_kernel, kv_n, heads_all, pos_here),
        out_shape=jax.ShapeDtypeStruct((seqs, cols), bf16),
        in_specs=[pl.BlockSpec(memory_space=pltpu.SMEM)] + [vmem] * 5 + [anywhere] * 9,
        out_specs=vmem,
        scratch_shapes=[
            pltpu.VMEM((cols, heads_all), bf16),
            pltpu.VMEM(w_query.shape, bf16),
            pltpu.VMEM(w_key.shape, bf16),
            pltpu.VMEM(w_value.shape, bf16),
            pltpu.VMEM(keys_cache.shape, bf16),
            pltpu.VMEM(values_cache.shape, bf16),
            pltpu.VMEM(w_out.shape, bf16),
            pltpu.VMEM(w_up.shape, bf16),
            pltpu.VMEM(w_down.shape, bf16),
            pltpu.VMEM((kv_n, 4 * rows, dim), bf16),
            pltpu.VMEM((others, 4 * rows, dim), bf16),
            pltpu.VMEM((kv_n, rows, dim), bf16),
            pltpu.VMEM((kv_n * rows, dim), f32),
            pltpu.VMEM((kv_n * rows, dim), f32),
            pltpu.VMEM((kv_n * rows, LANES), f32),
            pltpu.VMEM((kv_n, 2 * rows, dim), bf16),
            pltpu.VMEM((others, 2 * rows, dim), bf16),
            pltpu.VMEM((kv_n, rows, dim), f32),
            pltpu.VMEM((seqs, cols + LANES), f32),
            pltpu.VMEM((seqs, cols + LANES), f32),
            pltpu.VMEM((kv_n, seqs, hidden_here + LANES), bf16),
            pltpu.VMEM((others, seqs, hidden_here + LANES), bf16),
            pltpu.VMEM((kv_n, seqs, hidden_here), bf16),
            pltpu.VMEM((seqs, cols), f32),
            pltpu.VMEM((seqs, cols), f32),
            pltpu.SemaphoreType.DMA((7,)),
            pltpu.SemaphoreType.DMA((2, chunks)),
            pltpu.SemaphoreType.DMA((6, others)),
            pltpu.SemaphoreType.DMA((6, others)),
            pltpu.SemaphoreType.DMA((2,)),
            pltpu.SemaphoreType.DMA((2,)),
        ],
        compiler_params=pltpu.CompilerParams(
            collective_id=0, has_side_effects=True, vmem_limit_bytes=60 * 1024 * 1024
        ),
    )(
        lengths, stream, gain_in.reshape(1, -1), gain_att.reshape(1, -1),
        gain_mlp.reshape(1, -1), decay_cache,
        w_forget, w_query, w_key, w_value, keys_cache, values_cache, w_out, w_up, w_down,
    )


def solution(mesh):
    in_specs = (
        P(None, "kv"),
        P("kv"),
        P("kv", "tp"),
        P("kv", "tp"),
        P("kv", "tp"),
        P(),
        P(None, "tp", "kv", None),
        P(None, "tp", "kv", None),
        P(None, "tp", "kv"),
        P(),
        P("tp"),
        P("tp", "kv"),
        P("kv"),
        P("kv", "tp"),
        P("tp", "kv"),
    )
    out_specs = P(None, "kv")
    return jax.shard_map(
        layer, mesh=mesh, in_specs=in_specs, out_specs=out_specs, check_vma=False
    )
```

```python
import functools
import math

import jax
import jax.numpy as jnp
from jax import lax
from jax.experimental import pallas as pl
from jax.experimental.pallas import tpu as pltpu
from jax.sharding import PartitionSpec as P

f32 = jnp.float32
bf16 = jnp.bfloat16
LANES = 128

norm_eps = 1e-06
masked_score = -1e30


def merged_2(value, axis, join):
    pieces = jax.tree.map(lambda part: lax.all_gather(part, axis), value)
    head = jax.tree.map(lambda part: part[0], pieces)
    tail = jax.tree.map(lambda part: part[1:], pieces)
    so_far, _ = lax.scan(lambda so_far, share: (join(so_far, share), None), head, tail)
    return so_far


def fold_parts(left_part, right_part):
    peak_all = jnp.maximum(left_part[0], right_part[0])
    weight_one = jnp.exp(left_part[0] - peak_all)
    weight_two = jnp.exp(right_part[0] - peak_all)
    total_sum = left_part[1] * weight_one + right_part[1] * weight_two
    merged = left_part[2] * weight_one[..., None] + right_part[2] * weight_two[..., None]
    return (peak_all, total_sum, merged)


def per_device(
    stream,
    gain_in,
    w_query,
    w_key,
    w_value,
    w_forget,
    keys_cache,
    values_cache,
    decay_cache,
    lengths,
    gain_att,
    w_out,
    gain_mlp,
    w_up,
    w_down,
):
    kv_index = lax.axis_index("kv")
    tp_index = lax.axis_index("tp")
    kv_count = lax.axis_size("kv")
    seqs_here, cols_here = stream.shape
    heads_here = keys_cache.shape[1]
    pos_here = keys_cache.shape[2]
    head_dim = keys_cache.shape[3]
    width_all = cols_here * kv_count
    score_scale = 1.0 / math.sqrt(head_dim)
    stream_float = stream.astype(jnp.float32)
    scaled = (stream_float * gain_in.astype(jnp.float32)).astype(jnp.bfloat16)
    square_sum = jnp.sum(stream_float * stream_float, axis=1)
    forget_rows = lax.dynamic_slice(
        w_forget, (kv_index * cols_here, tp_index * heads_here), (cols_here, heads_here)
    )
    part_query = jnp.dot(scaled, w_query, preferred_element_type=jnp.float32)
    part_key = jnp.dot(scaled, w_key, preferred_element_type=jnp.float32)
    part_value = jnp.dot(scaled, w_value, preferred_element_type=jnp.float32)
    part_forget = jnp.dot(scaled, forget_rows, preferred_element_type=jnp.float32)
    part_query, part_key, part_value, part_forget, square_total = lax.psum(
        (part_query, part_key, part_value, part_forget, square_sum), "kv"
    )
    scale_in = lax.rsqrt(square_total / width_all + norm_eps)[:, None]
    queries = (part_query * scale_in).astype(jnp.bfloat16).reshape(seqs_here, heads_here, head_dim)
    key_new = (part_key * scale_in).astype(jnp.bfloat16).reshape(seqs_here, heads_here, head_dim)
    value_new = (
        (part_value * scale_in).astype(jnp.bfloat16).reshape(seqs_here, heads_here, head_dim)
    )
    forget = jax.nn.log_sigmoid(part_forget * scale_in)
    attention_logits = (
        jnp.einsum("shd,shpd->shp", queries, keys_cache, preferred_element_type=jnp.float32)
        * score_scale
    )
    attention_logits = attention_logits + forget[:, :, None] + decay_cache
    cache_positions = kv_index * pos_here + lax.iota(jnp.int32, pos_here)
    live_mask = (cache_positions[None, :] < lengths[:, None])[:, None, :]
    attention_logits = jnp.where(live_mask, attention_logits, masked_score)
    block_peak = jnp.max(attention_logits, axis=2)
    weights = jnp.where(live_mask, jnp.exp(attention_logits - block_peak[..., None]), 0.0)
    block_total = jnp.sum(weights, axis=2)
    block_out = jnp.einsum(
        "shp,shpd->shd",
        weights.astype(jnp.bfloat16),
        values_cache,
        preferred_element_type=jnp.float32,
    )
    peak_all, total_all, out_all = merged_2((block_peak, block_total, block_out), "kv", fold_parts)
    own_score = (
        jnp.sum(queries.astype(jnp.float32) * key_new.astype(jnp.float32), axis=2) * score_scale
    )
    top_score = jnp.maximum(peak_all, own_score)
    past_weight = jnp.exp(peak_all - top_score)
    own_weight = jnp.exp(own_score - top_score)
    numerator = (
        out_all * past_weight[..., None] + value_new.astype(jnp.float32) * own_weight[..., None]
    )
    denominator = total_all * past_weight + own_weight
    attended = (numerator / denominator[..., None]).reshape(seqs_here, heads_here * head_dim)
    attended_in = (attended * gain_att.astype(jnp.float32)).astype(jnp.bfloat16)
    part_out = jnp.dot(attended_in, w_out, preferred_element_type=jnp.float32)
    att_squares = jnp.sum(attended * attended, axis=1)
    part_out, att_total = lax.psum((part_out, att_squares), "tp")
    scale_att = lax.rsqrt(att_total / (attended.shape[1] * lax.axis_size("tp")) + norm_eps)[:, None]
    residual = (stream_float + scale_att * part_out).astype(jnp.bfloat16)
    residual_float = residual.astype(jnp.float32)
    mixer_in = (residual_float * gain_mlp.astype(jnp.float32)).astype(jnp.bfloat16)
    mixer_squares = jnp.sum(residual_float * residual_float, axis=1)
    part_up = jnp.dot(mixer_in, w_up, preferred_element_type=jnp.float32)
    pre_act, mixer_total = lax.psum((part_up, mixer_squares), "kv")
    scale_mixer = lax.rsqrt(mixer_total / width_all + norm_eps)[:, None]
    hidden = jnp.square(jax.nn.relu(pre_act * scale_mixer)).astype(jnp.bfloat16)
    part_down = jnp.dot(hidden, w_down, preferred_element_type=jnp.float32)
    mixer_out = lax.psum(part_down, "tp")
    return (residual_float + mixer_out).astype(jnp.bfloat16)


def thirds(value, group, wide):
    high = value.astype(bf16).astype(f32)
    rest = value - high
    mid = rest.astype(bf16).astype(f32)
    low = rest - mid
    third = group % 3 if wide else group
    picked = jnp.where(third == 0, high, jnp.where(third == 1, mid, low))
    return picked


def lanes_of(shape):
    return lax.broadcasted_iota(jnp.int32, shape, len(shape) - 1)


def layer_kernel(
    kv_n, heads_all, pos_here,
    lengths, stream, gain_in, gain_att, gain_mlp, decay,
    w_forget, w_query, w_key, w_value, keys, values, w_out, w_up, w_down,
    out,
    wf_v, wq_v, wk_v, wv_v, keys_v, values_v, wo_v, wu_v, wd_v,
    send1, recv1, q_all, q_float, o_float, s_float, send3, recv3, att_all,
    send5, recv5, send6, recv6, hid_all, send8, recv8,
    load_sem, cache_sem, ssem, rsem, pair_ssem, pair_rsem,
):
    me = lax.axis_index("kv")
    tp = lax.axis_index("tp")
    seqs, cols = stream.shape
    heads = decay.shape[1]
    dim = keys.shape[-1]
    rows = send1.shape[1] // 4
    groups = seqs // rows
    hidden_here = hid_all.shape[2]
    others = kv_n - 1
    chunks = cache_sem.shape[1]
    per_chunk = seqs // chunks
    score_scale = 1.0 / math.sqrt(dim)
    together = math.gcd(8, per_chunk)

    def load(src, dst, index):
        return pltpu.make_async_copy(src, dst, load_sem.at[index])

    start_row = pl.multiple_of(me * cols, cols)
    first_loads = [
        load(w_forget.at[:, pl.ds(start_row, cols)], wf_v, 0),
        load(w_query, wq_v, 1),
        load(w_key, wk_v, 2),
        load(w_value, wv_v, 3),
    ]
    for copy in first_loads:
        copy.start()

    def cache_copy(which, chunk):
        src, dst = ((keys, keys_v), (values, values_v))[which]
        part = pl.ds(chunk * per_chunk, per_chunk)
        return pltpu.make_async_copy(src.at[part], dst.at[part], cache_sem.at[which, chunk])

    late_loads = [load(w_out, wo_v, 4), load(w_up, wu_v, 5), load(w_down, wd_v, 6)]

    barrier = pltpu.get_barrier_semaphore()

    def greet(k, carry):
        pl.semaphore_signal(
            barrier, inc=1, device_id=(lax.rem(me + k, kv_n), tp),
            device_id_type=pl.DeviceIdType.MESH,
        )
        return carry

    lax.fori_loop(1, kv_n, greet, 0)
    pl.semaphore_signal(
        barrier, inc=1, device_id=(me, 1 - tp), device_id_type=pl.DeviceIdType.MESH
    )

    def partner(k):
        apart = kv_n - k
        bits = [1 << place for place in range(kv_n.bit_length() - 1)]
        return sum((((me // bit) + (apart // bit)) % 2) * bit for bit in bits)

    after = before = partner

    def remote(phase, k, src, dst):
        return pltpu.make_async_remote_copy(
            src_ref=src, dst_ref=dst,
            send_sem=ssem.at[phase, k - 1], recv_sem=rsem.at[phase, k - 1],
            device_id=(after(k), tp), device_id_type=pl.DeviceIdType.MESH,
        )

    def scatter(phase, k, send, recv):
        return remote(phase, k, send.at[after(k)], recv.at[k - 1])

    def spread(phase, k, held):
        return remote(phase, k, held.at[me], held.at[me])

    def landed(phase, k, held):
        return remote(phase, k, held.at[before(k)], held.at[before(k)])

    def each(body):
        lax.fori_loop(1, kv_n, lambda k, carry: (body(k), carry)[1], 0)

    def swap(index, src, dst):
        return pltpu.make_async_remote_copy(
            src_ref=src, dst_ref=dst, send_sem=pair_ssem.at[index],
            recv_sem=pair_rsem.at[index], device_id=(me, 1 - tp),
            device_id_type=pl.DeviceIdType.MESH,
        )

    x = stream[...].astype(f32)
    scaled = (x * gain_in[...].astype(f32).reshape(1, -1)).astype(bf16)
    squares = jnp.sum(x * x, axis=1, keepdims=True)
    for copy in first_loads:
        copy.wait()
    for chunk in range(chunks):
        cache_copy(0, chunk).start()
        cache_copy(1, chunk).start()
    for copy in late_loads:
        copy.start()
    lane = lanes_of((seqs, LANES))
    expand = lax.broadcasted_iota(jnp.int32, (heads_all, LANES), 0) == (
        lanes_of((heads_all, LANES)) % 32
    )
    wide_forget = lax.dot_general(
        wf_v[...], jnp.where(expand, 1.0, 0.0).astype(bf16), (((0,), (0,)), ((), ())),
        preferred_element_type=f32,
    ).astype(bf16)
    part_forget = jnp.dot(scaled, wide_forget, preferred_element_type=f32)
    stats = jnp.where(lane % 32 < heads_all, part_forget, squares)
    stats = thirds(stats, lane // 32, False)
    stats = jnp.where(lane < 96, stats, 0.0).astype(bf16)
    for place, weight in enumerate((wq_v, wk_v, wv_v)):
        part = jnp.dot(scaled, weight[...], preferred_element_type=f32).astype(bf16)
        for g in range(groups):
            for h in range(heads):
                send1[g * heads + h, place * rows:(place + 1) * rows, :] = part[
                    g * rows:(g + 1) * rows, h * dim:(h + 1) * dim
                ]
    for g in range(groups):
        for h in range(heads):
            send1[g * heads + h, 3 * rows:4 * rows, :] = stats[g * rows:(g + 1) * rows]
    pl.semaphore_wait(barrier, kv_n)
    each(lambda k: scatter(0, k, send1, recv1).start())

    def add1(k, total):
        scatter(0, k, send1, recv1).wait_recv()
        return total + recv1[k - 1].astype(f32)

    total = lax.fori_loop(1, kv_n, add1, send1[me].astype(f32))
    lane_r = lanes_of((rows, LANES))
    stat = total[3 * rows:]
    my_head = tp * heads + lax.rem(me, heads)
    forget_sum = jnp.sum(
        jnp.where(lane_r % 32 == my_head, stat, 0.0), axis=1, keepdims=True
    )
    square_sum = jnp.sum(
        jnp.where(lane_r % 32 == heads_all, stat, 0.0), axis=1, keepdims=True
    )
    width_all = cols * kv_n
    scale_in = lax.rsqrt(square_sum / width_all + norm_eps)
    query = (total[:rows] * scale_in).astype(bf16)
    key_new = (total[rows:2 * rows] * scale_in).astype(bf16).astype(f32)
    value_new = (total[2 * rows:3 * rows] * scale_in).astype(bf16).astype(f32)
    gate = forget_sum * scale_in
    forget = jnp.minimum(gate, 0.0) - jnp.log1p(jnp.exp(-jnp.abs(gate)))
    q_all[me] = query
    each(lambda k: spread(1, k, q_all).start())
    own_score = (
        jnp.sum(query.astype(f32) * key_new, axis=1, keepdims=True) * score_scale
    )
    each(lambda k: landed(1, k, q_all).wait_recv())

    q_float[...] = q_all[...].reshape(kv_n * rows, dim).astype(f32)
    head_row = lax.broadcasted_iota(jnp.int32, (heads, pos_here), 0)
    position = me * pos_here + lanes_of((heads, pos_here))
    lane_h = lanes_of((heads, LANES))

    def some_sequences(first_seq):
        batch = [first_seq + i for i in range(together)]
        places = [
            pl.ds((s // rows) * (heads * rows) + s % rows, heads, stride=rows) for s in batch
        ]
        q_parts = [q_float[mine, :].astype(bf16) for mine in places]
        everies = [
            lax.dot_general(
                q_s, keys_v[s].reshape(heads * pos_here, dim), (((1,), (1,)), ((), ())),
                preferred_element_type=f32,
            )
            for q_s, s in zip(q_parts, batch)
        ]
        spreads, stats = [], []
        for every, s in zip(everies, batch):
            score = every[:, :pos_here]
            for h in range(1, heads):
                score = jnp.where(
                    head_row == h, every[:, h * pos_here:(h + 1) * pos_here], score
                )
            score = score * score_scale + decay[s]
            live = position < lengths[s]
            score = jnp.where(live, score, masked_score)
            peak = jnp.max(score, axis=1, keepdims=True)
            probs = jnp.where(live, jnp.exp(score - peak), 0.0)
            block_total = jnp.sum(probs, axis=1, keepdims=True)
            spreads.append(jnp.concatenate(
                [jnp.where(head_row == h, probs, 0.0) for h in range(heads)], axis=1
            ).astype(bf16))
            stats.append(jnp.where(lane_h < 48, peak, block_total))
        outs = [
            jnp.dot(
                part, values_v[s].reshape(heads * pos_here, dim), preferred_element_type=f32
            )
            for part, s in zip(spreads, batch)
        ]
        for mine, out_s, stat_s in zip(places, outs, stats):
            o_float[mine, :] = out_s
            s_float[mine, :] = stat_s

    def one_chunk(chunk, carry):
        cache_copy(0, chunk).wait()
        cache_copy(1, chunk).wait()

        def inner(i, c):
            some_sequences(chunk * per_chunk + together * i)
            return c

        return lax.fori_loop(0, per_chunk // together, inner, carry)

    lax.fori_loop(0, chunks, one_chunk, 0)
    stats3 = s_float[...]
    stats3 = thirds(stats3, lanes_of(stats3.shape) // 16, True)
    send3[:, :rows, :] = o_float[...].astype(bf16).reshape(kv_n, rows, dim)
    send3[:, rows:, :] = stats3.astype(bf16).reshape(kv_n, rows, LANES)
    each(lambda k: scatter(2, k, send3, recv3).start())

    def opened(block):
        wide = block.astype(f32)
        stat = wide[rows:]
        is_third = lane_r % 16 == 0
        peak = jnp.sum(
            jnp.where(is_third & (lane_r < 48), stat, 0.0), axis=1, keepdims=True
        )
        total = jnp.sum(
            jnp.where(is_third & (lane_r >= 48) & (lane_r < 96), stat, 0.0),
            axis=1, keepdims=True,
        )
        return peak, total, wide[:rows]

    def fold3(k, so_far):
        scatter(2, k, send3, recv3).wait_recv()
        peak_a, total_a, out_a = so_far
        peak_b, total_b, out_b = opened(recv3[k - 1])
        peak = jnp.maximum(peak_a, peak_b)
        one, two = jnp.exp(peak_a - peak), jnp.exp(peak_b - peak)
        return peak, total_a * one + total_b * two, out_a * one + out_b * two

    peak_all, total_all, out_all = lax.fori_loop(1, kv_n, fold3, opened(send3[me]))
    peak_all = peak_all + forget
    top = jnp.maximum(peak_all, own_score)
    past_weight = jnp.exp(peak_all - top)
    own_weight = jnp.exp(own_score - top)
    att_all[me] = (out_all * past_weight + value_new * own_weight) / (
        total_all * past_weight + own_weight
    )
    each(lambda k: spread(3, k, att_all).start())
    each(lambda k: landed(3, k, att_all).wait_recv())
    attended = jnp.concatenate(
        [
            jnp.concatenate([att_all[g * heads + h] for g in range(groups)], axis=0)
            for h in range(heads)
        ],
        axis=1,
    )
    attended_in = (attended * gain_att[...].astype(f32).reshape(1, -1)).astype(bf16)
    late_loads[0].wait()
    part_out = jnp.dot(attended_in, wo_v[...], preferred_element_type=f32)
    att_squares = jnp.sum(attended * attended, axis=1, keepdims=True)
    send5[:, :cols] = part_out
    send5[:, cols:] = jnp.broadcast_to(att_squares, (seqs, LANES))
    swap5 = swap(0, send5, recv5)
    swap5.start()
    late_loads[1].wait()
    swap5.wait_recv()
    scale_att = lax.rsqrt(
        (att_squares + recv5[:, cols:cols + 1]) / (attended.shape[1] * 2) + norm_eps
    )
    residual = (
        stream[...].astype(f32) + scale_att * (part_out + recv5[:, :cols])
    ).astype(bf16).astype(f32)
    mixer_in = (residual * gain_mlp[...].astype(f32).reshape(1, -1)).astype(bf16)
    mixer_squares = jnp.sum(residual * residual, axis=1, keepdims=True)
    mixer_stats = thirds(jnp.broadcast_to(mixer_squares, (seqs, LANES)), lane, False)
    mixer_stats = jnp.where(lane < 3, mixer_stats, 0.0).astype(bf16)

    def up(owner):
        columns = pl.ds(pl.multiple_of(owner * hidden_here, LANES), hidden_here)
        send6[owner, :, :hidden_here] = jnp.dot(
            mixer_in, wu_v[:, columns], preferred_element_type=f32
        ).astype(bf16)
        send6[owner, :, hidden_here:] = mixer_stats

    def up_send(k):
        up(after(k))
        scatter(4, k, send6, recv6).start()

    each(up_send)
    up(me)

    def add6(k, total):
        scatter(4, k, send6, recv6).wait_recv()
        return total + recv6[k - 1].astype(f32)

    pre_act = lax.fori_loop(1, kv_n, add6, send6[me].astype(f32))
    mixer_total = jnp.sum(pre_act[:, hidden_here:], axis=1, keepdims=True)
    scale_mixer = lax.rsqrt(mixer_total / width_all + norm_eps)
    hidden = jnp.maximum(pre_act[:, :hidden_here] * scale_mixer, 0.0)
    hid_all[me] = (hidden * hidden).astype(bf16)
    each(lambda k: spread(5, k, hid_all).start())
    late_loads[2].wait()

    def down(owner):
        depth = pl.ds(pl.multiple_of(owner * hidden_here, LANES), hidden_here)
        return jnp.dot(hid_all[owner], wd_v[depth, :], preferred_element_type=f32)

    def add7(k, total):
        landed(5, k, hid_all).wait_recv()
        return total + down(before(k))

    part_down = lax.fori_loop(1, kv_n, add7, down(me))
    send8[...] = part_down
    swap8 = swap(1, send8, recv8)
    swap8.start()
    swap8.wait_recv()
    out[...] = (residual + (part_down + recv8[...])).astype(bf16)

    def drain(k):
        scatter(0, k, send1, recv1).wait_send()
        spread(1, k, q_all).wait_send()
        scatter(2, k, send3, recv3).wait_send()
        spread(3, k, att_all).wait_send()
        scatter(4, k, send6, recv6).wait_send()
        spread(5, k, hid_all).wait_send()

    each(drain)
    swap5.wait_send()
    swap8.wait_send()


def fits(kv_n, tp_n, seqs, cols, heads, heads_all, pos_here, dim, units):
    if tp_n != 2 or heads != 8 or (seqs * heads) % kv_n or units % kv_n or seqs % 32:
        return False
    rows = seqs * heads // kv_n
    return (
        rows % 16 == 0 and 4 % max(1, seqs // rows) == 0 and seqs % rows == 0
        and kv_n & (kv_n - 1) == 0 and cols % LANES == 0
        and pos_here == LANES and dim == LANES and heads_all <= 16
        and (units // kv_n) % LANES == 0
    )


def layer(
    stream, gain_in, w_query, w_key, w_value, w_forget, keys_cache, values_cache,
    decay_cache, lengths, gain_att, w_out, gain_mlp, w_up, w_down,
):
    kv_n, tp_n = lax.axis_size("kv"), lax.axis_size("tp")
    seqs, cols = stream.shape
    heads, pos_here, dim = keys_cache.shape[1:]
    heads_all = w_forget.shape[1]
    units = w_up.shape[1]
    if not fits(kv_n, tp_n, seqs, cols, heads, heads_all, pos_here, dim, units):
        return per_device(
            stream, gain_in, w_query, w_key, w_value, w_forget, keys_cache, values_cache,
            decay_cache, lengths, gain_att, w_out, gain_mlp, w_up, w_down,
        )
    rows = seqs * heads // kv_n
    hidden_here = units // kv_n
    others = kv_n - 1
    chunks = 4
    vmem = pl.BlockSpec(memory_space=pltpu.VMEM)
    anywhere = pl.BlockSpec(memory_space=pl.ANY)
    return pl.pallas_call(
        functools.partial(layer_kernel, kv_n, heads_all, pos_here),
        out_shape=jax.ShapeDtypeStruct((seqs, cols), bf16),
        in_specs=[pl.BlockSpec(memory_space=pltpu.SMEM)] + [vmem] * 5 + [anywhere] * 9,
        out_specs=vmem,
        scratch_shapes=[
            pltpu.VMEM((heads_all, cols), bf16),
            pltpu.VMEM(w_query.shape, bf16),
            pltpu.VMEM(w_key.shape, bf16),
            pltpu.VMEM(w_value.shape, bf16),
            pltpu.VMEM(keys_cache.shape, bf16),
            pltpu.VMEM(values_cache.shape, bf16),
            pltpu.VMEM(w_out.shape, bf16),
            pltpu.VMEM(w_up.shape, bf16),
            pltpu.VMEM(w_down.shape, bf16),
            pltpu.VMEM((kv_n, 4 * rows, dim), bf16),
            pltpu.VMEM((others, 4 * rows, dim), bf16),
            pltpu.VMEM((kv_n, rows, dim), bf16),
            pltpu.VMEM((kv_n * rows, dim), f32),
            pltpu.VMEM((kv_n * rows, dim), f32),
            pltpu.VMEM((kv_n * rows, LANES), f32),
            pltpu.VMEM((kv_n, 2 * rows, dim), bf16),
            pltpu.VMEM((others, 2 * rows, dim), bf16),
            pltpu.VMEM((kv_n, rows, dim), f32),
            pltpu.VMEM((seqs, cols + LANES), f32),
            pltpu.VMEM((seqs, cols + LANES), f32),
            pltpu.VMEM((kv_n, seqs, hidden_here + LANES), bf16),
            pltpu.VMEM((others, seqs, hidden_here + LANES), bf16),
            pltpu.VMEM((kv_n, seqs, hidden_here), bf16),
            pltpu.VMEM((seqs, cols), f32),
            pltpu.VMEM((seqs, cols), f32),
            pltpu.SemaphoreType.DMA((7,)),
            pltpu.SemaphoreType.DMA((2, chunks)),
            pltpu.SemaphoreType.DMA((6, others)),
            pltpu.SemaphoreType.DMA((6, others)),
            pltpu.SemaphoreType.DMA((2,)),
            pltpu.SemaphoreType.DMA((2,)),
        ],
        compiler_params=pltpu.CompilerParams(
            collective_id=0, has_side_effects=True, vmem_limit_bytes=60 * 1024 * 1024
        ),
    )(
        lengths, stream, gain_in, gain_att,
        gain_mlp, decay_cache,
        w_forget.T, w_query, w_key, w_value, keys_cache, values_cache, w_out, w_up, w_down,
    )


def solution(mesh):
    in_specs = (
        P(None, "kv"),
        P("kv"),
        P("kv", "tp"),
        P("kv", "tp"),
        P("kv", "tp"),
        P(),
        P(None, "tp", "kv", None),
        P(None, "tp", "kv", None),
        P(None, "tp", "kv"),
        P(),
        P("tp"),
        P("tp", "kv"),
        P("kv"),
        P("kv", "tp"),
        P("tp", "kv"),
    )
    out_specs = P(None, "kv")
    return jax.shard_map(
        layer, mesh=mesh, in_specs=in_specs, out_specs=out_specs, check_vma=False
    )
```
